32 devices in a mesh: rep: 1, fs: 8 (over z, y), tp: 4 (over x, core).
Axes of the slice: x: 2, y: 2, z: 4, core: 2. Of those that a mesh axis runs over, the one named last changes fastest.
Arguments:
- tokens: bfloat16 [4096, 2048], P(('rep', 'fs')), may hold values from -6 to 6
- gate_outer: bfloat16 [2048, 1024], P('fs', 'tp'), may hold values from -0.125 to 0.125
- gate_inner: bfloat16 [2048, 1024], P('fs', 'tp'), may hold values from -0.125 to 0.125
- conv_input: bfloat16 [2048, 1024], P('fs', 'tp'), may hold values from -0.125 to 0.125
- mixer_output: bfloat16 [2048, 1024], P('fs', 'tp'), may hold values from -0.1875 to 0.1875
- conv_taps: float32 [3, 1024], P(None, 'tp'), may hold values from -3 to 3
- mixer_gain: float32 [2048], replicated, may hold values from 0.1 to 1.9
- mixer_shift: float32 [2048], replicated, may hold values from -3 to 3
- up_weight: bfloat16 [2048, 8192], P('fs', 'tp'), may hold values from -0.125 to 0.125
- down_weight: bfloat16 [2048, 8192], P('fs', 'tp'), may hold values from -0.0625 to 0.0625
- channel_gain: float32 [2048], replicated, may hold values from 0.1 to 1.9
- channel_shift: float32 [2048], replicated, may hold values from -3 to 3
Outputs:
- mixed: bfloat16 [4096, 2048], P(('rep', 'fs'))
The draws below stay inside these ranges and needn't reach their ends.
All inputs are finite; a program needn't handle non-finite values.
Results may differ from the reference program's by a relative error of at most 0.014.
Values may be sent and summed in bfloat16 or wider, within the bound.
No kernel may reach another device: no remote copies, remote signals or barrier semaphores. Data moves between devices by JAX's collectives and lax.ppermute only.
A program may use at most 64 MiB of HBM per device.

```python
import jax
import jax.numpy as jnp
from jax import lax

D = 2048
C = 1024
FF = 8192
TAPS = 3
LEN = 512
SEQS = 8
TOKENS = 4096
N_TP = 4


def levels(rng, dims, shards, least, top_value):
    loudness = 1.0
    for axis_at, parts in shards:
        steps = jax.random.uniform(jax.random.fold_in(jax.random.fold_in(rng, 6), axis_at), (parts,), jnp.float32, least / len(shards), top_value / len(shards))
        loudness = loudness * jnp.repeat(jnp.exp(steps), dims[axis_at] // parts).reshape((-1,) + (1,) * (len(dims) - 1 - axis_at))
    return loudness


def bell_draw(own_key, dims, deviation, most, pieces=(), dtype=jnp.bfloat16):
    drawn = jax.random.normal(own_key, dims, jnp.float32) * deviation
    if len(pieces) > 0:
        drawn = levels(own_key, dims, pieces, -0.22, 0.18) * drawn
    return jnp.clip(drawn, min=-most, max=most).astype(dtype)


def setup_inputs(seed: int = 0) -> dict:
    arg_keys = jax.random.split(jax.random.key(seed), 13)
    return {
        "tokens": bell_draw(arg_keys[0], (TOKENS, D), 1.0, 6.0, ((0, 8),)),
        "gate_outer": bell_draw(arg_keys[1], (D, C), D ** -0.5, 0.125, ((0, 8), (1, 4))),
        "gate_inner": bell_draw(arg_keys[2], (D, C), D ** -0.5, 0.125, ((0, 8), (1, 4))),
        "conv_input": bell_draw(arg_keys[3], (D, C), D ** -0.5, 0.125, ((0, 8), (1, 4))),
        "mixer_output": bell_draw(arg_keys[4], (D, C), C ** -0.5, 0.1875, ((0, 8), (1, 4))),
        "conv_taps": bell_draw(arg_keys[5], (TAPS, C), 0.6, 3.0, ((1, 4),), jnp.float32),
        "mixer_gain": jnp.clip(1.0 + 0.18 * jax.random.normal(arg_keys[6], (D,), jnp.float32), 0.1, 1.9),
        "mixer_shift": bell_draw(arg_keys[7], (D,), 0.5, 3.0, (), jnp.float32),
        "up_weight": bell_draw(arg_keys[8], (D, FF), D ** -0.5, 0.125, ((0, 8), (1, 4))),
        "down_weight": bell_draw(arg_keys[9], (D, FF), FF ** -0.5, 0.0625, ((0, 8), (1, 4))),
        "channel_gain": jnp.clip(1.0 + 0.18 * jax.random.normal(arg_keys[10], (D,), jnp.float32), 0.1, 1.9),
        "channel_shift": bell_draw(arg_keys[11], (D,), 0.5, 3.0, (), jnp.float32),
    }


residual_scale = 8.0 ** 0.25
norm_epsilon = 1e-05

def layer_norm(values, gain, shift):
    row_mean = lax.optimization_barrier(jnp.mean(values, -1, keepdims=True))
    centered = values - row_mean
    variance = lax.optimization_barrier(jnp.mean(centered * centered, -1, keepdims=True))
    return centered * lax.rsqrt(variance + norm_epsilon) * gain + shift

def blockwise_sum(left, right_t):
    block_width = left.shape[1] // N_TP
    totals = jnp.zeros((left.shape[0], right_t.shape[0]), jnp.float32)
    for block_index in range(N_TP):
        lower = block_index * block_width
        product = lax.dot_general(left[:, lower:lower + block_width], right_t[:, lower:lower + block_width], (((1,), (1,)), ((), ())), preferred_element_type=jnp.float32)
        totals = totals + lax.optimization_barrier(product.astype(jnp.bfloat16)).astype(jnp.float32)
    return totals

def reference(tokens, gate_outer, gate_inner, conv_input, mixer_output, conv_taps, mixer_gain, mixer_shift, up_weight, down_weight, channel_gain, channel_shift):

    def one_sequence(seq_rows):
        outer_gate = jnp.dot(seq_rows, gate_outer, preferred_element_type=jnp.float32)
        inner_gate = jnp.dot(seq_rows, gate_inner, preferred_element_type=jnp.float32)
        conv_values = jnp.dot(seq_rows, conv_input, preferred_element_type=jnp.float32)
        product = inner_gate * conv_values
        padded = jnp.pad(product, ((TAPS - 1, 0), (0, 0)))
        result = jnp.zeros_like(product)
        for tap_index in range(TAPS):
            result = result + conv_taps[tap_index] * padded[tap_index:tap_index + LEN]
        conv_out = (outer_gate * result).astype(jnp.bfloat16)
        mixer_sum = blockwise_sum(conv_out, mixer_output)
        first = layer_norm(residual_scale * seq_rows.astype(jnp.float32) + mixer_sum, mixer_gain, mixer_shift).astype(jnp.bfloat16)
        up_product = jnp.dot(first, up_weight, preferred_element_type=jnp.float32)
        hidden = jnp.square(jax.nn.relu(up_product)).astype(jnp.bfloat16)
        channel_sum = blockwise_sum(hidden, down_weight)
        return layer_norm(residual_scale * first.astype(jnp.float32) + channel_sum, channel_gain, channel_shift).astype(jnp.bfloat16)
    sequences = tokens.reshape(SEQS, LEN, D)
    outputs = lax.map(one_sequence, sequences)
    return outputs.reshape(TOKENS, D)
```

```python
import jax
import jax.numpy as jnp
from jax import lax
from jax.sharding import PartitionSpec as P

residual_scale = 8.0**0.25
norm_epsilon = 1e-05


def layer_norm(values, gain, shift):
    row_mean = jnp.mean(values, -1, keepdims=True)
    centered = values - row_mean
    variance = jnp.mean(centered * centered, -1, keepdims=True)
    return centered * lax.rsqrt(variance + norm_epsilon) * gain + shift


def grid_cycle(count, width):
    if width < 2 or count % width or (count // width) % 2:
        return list(range(count))
    rows = count // width
    order = [row * width for row in range(rows)]
    for step, row in enumerate(reversed(range(rows))):
        others = list(range(1, width))
        if step % 2:
            others.reverse()
        order += [row * width + column for column in others]
    return order


def after(value, *earlier):
    return lax.optimization_barrier((value,) + earlier)[0]


class Ring:
    def __init__(self, axis, order):
        self.axis = axis
        self.count = len(order)
        self.up = [(order[i], order[(i + 1) % self.count]) for i in range(self.count)]
        self.down = [(b, a) for a, b in self.up]
        table = [None] * self.count
        for at, member in enumerate(order):
            table[member] = [order[(at + k) % self.count] for k in range(self.count)]
        row = lax.axis_index(axis)
        self.members = lax.dynamic_index_in_dim(
            jnp.array(table, jnp.int32), row, 0, keepdims=False
        )

    def member(self, offset):
        return self.members[offset % self.count]

    def gather(self, shard):
        if self.count > 8:
            full = lax.all_gather(shard, self.axis, axis=0, tiled=True)
            half = full.shape[0] // 2
            return [(jnp.int32(0), (full[:half], full[half:]))]
        half = shard.shape[0] // 2
        pieces = (shard[:half], shard[half:])
        arrivals = [(self.member(0), pieces)]
        ahead = list(pieces)
        behind = list(pieces)
        for step in range(1, (self.count - 1) // 2 + 1):
            for at in range(2):
                ahead[at] = lax.ppermute(ahead[at], self.axis, self.up)
                behind[at] = lax.ppermute(behind[at], self.axis, self.down)
            arrivals.append((self.member(-step), tuple(ahead)))
            arrivals.append((self.member(step), tuple(behind)))
        if self.count % 2 == 0:
            last = (
                lax.ppermute(ahead[0], self.axis, self.up),
                lax.ppermute(behind[1], self.axis, self.down),
            )
            arrivals.append((self.member(self.count // 2), last))
        return arrivals


def swap(value, bit):
    size = lax.axis_size("tp")
    return lax.ppermute(value, "tp", [(i, i ^ bit) for i in range(size)])


def rounded(value):
    return lax.optimization_barrier(value.astype(jnp.bfloat16))


def add_rounded(left, right):
    return rounded(left.astype(jnp.float32) + right.astype(jnp.float32))


def tp_sum(partial):
    size = lax.axis_size("tp")
    total = rounded(partial)
    bit = 1
    while bit < size:
        other = swap(total, bit)
        if 2 * bit < size:
            total = add_rounded(total, other)
        else:
            return total.astype(jnp.float32) + other.astype(jnp.float32)
        bit *= 2
    return total.astype(jnp.float32)


def gated_conv(outer_gate, inner_gate, conv_values, conv_taps):
    seq_len = conv_values.shape[0]
    tap_count = conv_taps.shape[0]
    product = inner_gate * conv_values
    padded = jnp.pad(product, ((tap_count - 1, 0), (0, 0)))
    result = jnp.zeros_like(product)
    for tap_index in range(tap_count):
        result = result + conv_taps[tap_index] * padded[tap_index : tap_index + seq_len]
    return (outer_gate * result).astype(jnp.bfloat16)


def matmul_t(left, right_t):
    return lax.dot_general(
        left, right_t, (((1,), (1,)), ((), ())), preferred_element_type=jnp.float32
    )


def local(
    tokens,
    gate_outer,
    gate_inner,
    conv_input,
    mixer_output,
    conv_taps,
    mixer_gain,
    mixer_shift,
    up_weight,
    down_weight,
    channel_gain,
    channel_shift,
):
    features = tokens.shape[1]
    width = mixer_gain.shape[0] // lax.axis_size("fs")
    channels = gate_outer.shape[1]
    ring = Ring("fs", grid_cycle(lax.axis_size("fs"), lax.axis_size("tp") // 2))

    mixer_pack = jnp.concatenate([gate_outer, gate_inner, conv_input, mixer_output], axis=1)
    mixer_shards = ring.gather(mixer_pack)
    mixer_mark = mixer_shards[-2:][0][1][1][:8, :128]
    up_shards = ring.gather(after(up_weight, mixer_mark))
    up_mark = up_shards[-2:][0][1][1][:8, :128]
    down_shards = ring.gather(after(down_weight, up_mark))

    mixer_full = jnp.zeros((features, 4 * channels), jnp.bfloat16)
    for member, (low, high) in mixer_shards:
        mixer_full = lax.dynamic_update_slice(mixer_full, low, (member * width, 0))
        mixer_full = lax.dynamic_update_slice(
            mixer_full, high, (member * width + low.shape[0], 0)
        )
    projected = jnp.dot(
        tokens, mixer_full[:, : 3 * channels], preferred_element_type=jnp.float32
    )
    conv_out = gated_conv(
        projected[:, :channels],
        projected[:, channels : 2 * channels],
        projected[:, 2 * channels :],
        conv_taps,
    )
    mixer_sum = tp_sum(matmul_t(conv_out, mixer_full[:, 3 * channels :]))
    first = layer_norm(
        residual_scale * tokens.astype(jnp.float32) + mixer_sum, mixer_gain, mixer_shift
    ).astype(jnp.bfloat16)

    up_product = None
    for member, pieces in up_shards:
        rows = jnp.concatenate(pieces, axis=0)
        columns = lax.dynamic_slice_in_dim(first, member * width, rows.shape[0], 1)
        term = jnp.dot(columns, rows, preferred_element_type=jnp.float32)
        up_product = term if up_product is None else up_product + term
    hidden = jnp.square(jax.nn.relu(up_product)).astype(jnp.bfloat16)

    channel_sum = jnp.zeros(tokens.shape, jnp.float32)
    for member, pieces in down_shards:
        part = tp_sum(matmul_t(hidden, jnp.concatenate(pieces, axis=0)))
        channel_sum = lax.dynamic_update_slice(channel_sum, part, (0, member * width))
    return layer_norm(
        residual_scale * first.astype(jnp.float32) + channel_sum, channel_gain, channel_shift
    ).astype(jnp.bfloat16)


def solution(mesh):
    in_specs = (
        P(("rep", "fs"), None),
        P("fs", "tp"),
        P("fs", "tp"),
        P("fs", "tp"),
        P("fs", "tp"),
        P(None, "tp"),
        P(),
        P(),
        P("fs", "tp"),
        P("fs", "tp"),
        P(),
        P(),
    )
    out_specs = P(("rep", "fs"), None)
    return jax.shard_map(local, mesh=mesh, in_specs=in_specs, out_specs=out_specs, check_vma=False)
```

```python
import jax
import jax.numpy as jnp
from jax import lax
from jax.sharding import PartitionSpec as P


residual_scale = 8.0**0.25
norm_epsilon = 1e-05


def layer_norm(values, gain, shift):
    row_mean = jnp.mean(values, -1, keepdims=True)
    centered = values - row_mean
    variance = jnp.mean(centered * centered, -1, keepdims=True)
    return centered * lax.rsqrt(variance + norm_epsilon) * gain + shift


def grid_cycle(count, width):
    if width < 2 or count % width or (count // width) % 2:
        return list(range(count))
    rows = count // width
    order = [row * width for row in range(rows)]
    for step, row in enumerate(reversed(range(rows))):
        others = list(range(1, width))
        if step % 2:
            others.reverse()
        order += [row * width + column for column in others]
    return order


class Ring:
    def __init__(self, axis, order):
        self.axis = axis
        self.count = len(order)
        self.up = [(order[i], order[(i + 1) % self.count]) for i in range(self.count)]
        self.down = [(b, a) for a, b in self.up]
        table = [None] * self.count
        for at, member in enumerate(order):
            table[member] = [order[(at + k) % self.count] for k in range(self.count)]
        row = lax.axis_index(axis)
        self.members = lax.dynamic_index_in_dim(
            jnp.array(table, jnp.int32), row, 0, keepdims=False
        )

    def member(self, offset):
        return self.members[offset % self.count]

    def send(self, value, way):
        pairs = self.up if way == "f" else self.down
        return lax.ppermute(value, self.axis, pairs)

    def gather(self, shard):
        if self.count > 8:
            return [[(jnp.int32(0), lax.all_gather(shard, self.axis, axis=0, tiled=True))]]
        half = shard.shape[0] // 2
        ahead = [shard[:half], shard[half:]]
        behind = list(ahead)
        groups = [[(self.member(0), shard)]]
        for step in range(1, (self.count - 1) // 2 + 1):
            for at in range(2):
                ahead[at] = self.send(ahead[at], "f")
                behind[at] = self.send(behind[at], "b")
            groups.append(
                [
                    (self.member(-step), jnp.concatenate(ahead, axis=0)),
                    (self.member(step), jnp.concatenate(behind, axis=0)),
                ]
            )
        if self.count % 2 == 0:
            step = self.count // 2
            last = [self.send(ahead[0], "f"), self.send(behind[1], "b")]
            groups.append([(self.member(step), jnp.concatenate(last, axis=0))])
        return groups


def swap(value, bit):
    size = lax.axis_size("tp")
    return lax.ppermute(value, "tp", [(i, i ^ bit) for i in range(size)])


def rounded(value):
    return lax.optimization_barrier(value.astype(jnp.bfloat16))


def add_rounded(left, right):
    return rounded(left.astype(jnp.float32) + right.astype(jnp.float32))


def tp_sum(partial):
    size = lax.axis_size("tp")
    total = rounded(partial)
    bit = 1
    while bit < size:
        total = add_rounded(total, swap(total, bit))
        bit *= 2
    return total.astype(jnp.float32)


def tp_sum_halved(partial):
    size = lax.axis_size("tp")
    if size < 2:
        return tp_sum(partial)
    total = rounded(partial)
    half = total.shape[0] // 2
    odd = lax.axis_index("tp") % 2
    mine = lax.dynamic_slice_in_dim(total, odd * half, half, 0)
    other = lax.dynamic_slice_in_dim(total, (1 - odd) * half, half, 0)
    mine = add_rounded(mine, swap(other, 1))
    bit = 2
    while bit < size:
        mine = add_rounded(mine, swap(mine, bit))
        bit *= 2
    other = lax.ppermute(mine, "tp", [(i, i ^ 1) for i in range(size)])
    total = lax.dynamic_update_slice_in_dim(total, mine, odd * half, 0)
    total = lax.dynamic_update_slice_in_dim(total, other, (1 - odd) * half, 0)
    return total.astype(jnp.float32)


def gated_conv(outer_gate, inner_gate, conv_values, conv_taps):
    seq_len = conv_values.shape[0]
    tap_count = conv_taps.shape[0]
    product = inner_gate * conv_values
    padded = jnp.pad(product, ((tap_count - 1, 0), (0, 0)))
    result = jnp.zeros_like(product)
    for tap_index in range(tap_count):
        result = result + conv_taps[tap_index] * padded[tap_index : tap_index + seq_len]
    return (outer_gate * result).astype(jnp.bfloat16)


def matmul_t(left, right_t):
    return lax.dot_general(
        left, right_t, (((1,), (1,)), ((), ())), preferred_element_type=jnp.float32
    )


def local(
    tokens,
    gate_outer,
    gate_inner,
    conv_input,
    mixer_output,
    conv_taps,
    mixer_gain,
    mixer_shift,
    up_weight,
    down_weight,
    channel_gain,
    channel_shift,
):
    features = tokens.shape[1]
    width = mixer_gain.shape[0] // lax.axis_size("fs")
    channels = gate_outer.shape[1]
    ring = Ring("fs", grid_cycle(lax.axis_size("fs"), lax.axis_size("tp") // 2))

    mixer_pack = jnp.concatenate([gate_outer, gate_inner, conv_input, mixer_output], axis=1)
    mixer_groups = ring.gather(mixer_pack)
    up_groups = ring.gather(up_weight)
    down_groups = ring.gather(down_weight)

    mixer_full = jnp.zeros((features, 4 * channels), jnp.bfloat16)
    for group in mixer_groups:
        for member, rows in group:
            mixer_full = lax.dynamic_update_slice(mixer_full, rows, (member * width, 0))
    projected = jnp.dot(tokens, mixer_full[:, : 3 * channels], preferred_element_type=jnp.float32)
    conv_out = gated_conv(
        projected[:, :channels],
        projected[:, channels : 2 * channels],
        projected[:, 2 * channels :],
        conv_taps,
    )
    mixer_sum = tp_sum_halved(matmul_t(conv_out, mixer_full[:, 3 * channels :]))
    first = layer_norm(
        residual_scale * tokens.astype(jnp.float32) + mixer_sum, mixer_gain, mixer_shift
    ).astype(jnp.bfloat16)

    up_product = None
    for group in up_groups:
        for member, rows in group:
            columns = lax.dynamic_slice_in_dim(first, member * width, rows.shape[0], 1)
            term = jnp.dot(columns, rows, preferred_element_type=jnp.float32)
            up_product = term if up_product is None else up_product + term
    hidden = jnp.square(jax.nn.relu(up_product)).astype(jnp.bfloat16)

    channel_sum = jnp.zeros(tokens.shape, jnp.float32)
    for group in down_groups:
        rows = jnp.concatenate([rows for _, rows in group], axis=0)
        part = matmul_t(hidden, rows)
        part = tp_sum(part)
        start = 0
        for member, rows in group:
            piece = part[:, start : start + rows.shape[0]]
            channel_sum = lax.dynamic_update_slice(channel_sum, piece, (0, member * width))
            start += rows.shape[0]
    return layer_norm(
        residual_scale * first.astype(jnp.float32) + channel_sum, channel_gain, channel_shift
    ).astype(jnp.bfloat16)


def solution(mesh):
    in_specs = (
        P(("rep", "fs"), None),
        P("fs", "tp"),
        P("fs", "tp"),
        P("fs", "tp"),
        P("fs", "tp"),
        P(None, "tp"),
        P(),
        P(),
        P("fs", "tp"),
        P("fs", "tp"),
        P(),
        P(),
    )
    out_specs = P(("rep", "fs"), None)


    return jax.shard_map(local, mesh=mesh, in_specs=in_specs, out_specs=out_specs, check_vma=False)
```
